32 devices in a mesh: sp: 8 (over z, y), tp: 4 (over x, core).
Axes of the slice: x: 2, y: 2, z: 4, core: 2. Of those that a mesh axis runs over, the one named last changes fastest.
Arguments:
- tokens: bfloat16 [3072, 2048], P('sp'), may hold values from -6 to 6
- in_gain: float32 [2048], replicated, may hold values from 0.1 to 1.9
- query_weight: bfloat16 [2048, 1024], P(None, 'tp'), may hold values from -0.125 to 0.125
- key_weight: bfloat16 [2048, 1024], P(None, 'tp'), may hold values from -0.125 to 0.125
- value_weight: bfloat16 [2048, 2048], P(None, 'tp'), may hold values from -0.125 to 0.125
- gate_weight: bfloat16 [2048, 2048], P(None, 'tp'), may hold values from -0.125 to 0.125
- decay_down: bfloat16 [2048, 32], replicated, may hold values from -0.125 to 0.125
- decay_up: bfloat16 [32, 1024], replicated, may hold values from -1 to 1
- decay_offset: float32 [1024], P('tp')
- decay_extra: float32 [3072, 1024], P('sp', 'tp'), may hold values from -2 to 0, as said below
- head_gain: float32 [2048], P('tp'), may hold values from 0.1 to 1.9
- out_weight: bfloat16 [2048, 2048], P(None, 'tp'), may hold values from -4 to 4
- out_gain: float32 [2048], P('tp'), may hold values from 0.1 to 1.9
Outputs:
- layer_output: bfloat16 [3072, 2048], P('sp', 'tp')
The draws below stay inside these ranges and needn't reach their ends.
Inputs may be any that keep to these rules, and one draw needn't show every extreme that they name: `decay_extra`: never positive.
All inputs are finite; a program needn't handle non-finite values.
Results may differ from the reference program's by a relative error of at most 0.015.
Values may be sent and summed in bfloat16 or wider, within the bound.
No kernel may reach another device: no remote copies, remote signals or barrier semaphores. Data moves between devices by JAX's collectives and lax.ppermute only.
A program may use at most 64 MiB of HBM per device.

```python
import math
import jax
import jax.numpy as jnp
from jax import lax

D = 2048
ATTENTION_UNITS = 8
QUERY_FEATURES = 128
DV = 256
RANK = 32
BLOCK = 64
TOK = 384
TOKEN_SPAN = 3072
KW = 1024
VW = 2048


def draw_decay_offset(key, part):
    base_key = jax.random.fold_in(key, 11)
    order_key, jitter_key = jax.random.split(base_key)
    jitter = jax.random.uniform(jitter_key, (ATTENTION_UNITS, QUERY_FEATURES), jnp.float32, -0.5, 0.5)
    slow_level = math.log(4.0 * TOKEN_SPAN / 16.0)
    ranking = jax.random.permutation(order_key, ATTENTION_UNITS)
    slow_heads = (ranking < ATTENTION_UNITS // 2)[:, None]
    levels = jnp.where(slow_heads, slow_level, 0.0) + jitter
    return levels.reshape(ATTENTION_UNITS * QUERY_FEATURES).astype(jnp.float32)


def draw_decay_extra(key, part):
    base_key = jax.random.fold_in(key, 23)
    rate_key, channel_key, place_key, depth_key = jax.random.split(base_key, 4)
    block_total = TOKEN_SPAN // TOK
    block_rates = jnp.exp(jax.random.uniform(rate_key, (block_total, 1, ATTENTION_UNITS, 1), jnp.float32, math.log(0.1), math.log(2.0)))
    channel_rates = jnp.exp(jax.random.uniform(channel_key, (1, 1, ATTENTION_UNITS, QUERY_FEATURES), jnp.float32, math.log(0.5), math.log(2.0)))
    constant_amount = jnp.broadcast_to(-(block_rates * channel_rates) / TOKEN_SPAN, (block_total, TOK, ATTENTION_UNITS, QUERY_FEATURES))
    location_cells = jax.random.randint(place_key, (2, ATTENTION_UNITS), 0, TOKEN_SPAN)
    layer_tiers = jax.random.uniform(depth_key, (2, ATTENTION_UNITS), jnp.float32, math.log(0.5), math.log(0.8))
    token_ordinal = jnp.arange(TOKEN_SPAN)[:, None, None]
    packet_clusters = jnp.sum(jnp.where(token_ordinal == location_cells[None], layer_tiers[None], 0.0), axis=1)
    overall_number = constant_amount.reshape(TOKEN_SPAN, ATTENTION_UNITS, QUERY_FEATURES) + packet_clusters[:, :, None]
    return overall_number.reshape(TOKEN_SPAN, ATTENTION_UNITS * QUERY_FEATURES).astype(jnp.float32)


def draw_out_weight(key, part):
    base_key = jax.random.fold_in(key, 37)
    weight_key, jitter_key = jax.random.split(base_key)
    values = jax.random.truncated_normal(weight_key, -4.0, 4.0, (VW, D), jnp.float32) / math.sqrt(VW)
    columns = jnp.arange(D).astype(jnp.float32) / D
    jitter = jax.random.uniform(jitter_key, (D,), jnp.float32, 0.0, 1.0)
    exponent = (columns + jitter / 8.0) / 1.125
    return (values * jnp.power(10.0, exponent)[None, :]).astype(jnp.bfloat16)


def steps_of(rng, extent, shards, smallest, largest):
    loudness, own = 1.0, jax.random.fold_in(rng, 6)
    for dim, shards_of in shards:
        draws = jnp.exp(jax.random.uniform(jax.random.fold_in(own, dim), (shards_of,), jnp.float32, smallest / len(shards), largest / len(shards)))
        loudness = loudness * jnp.repeat(draws, extent[dim] // shards_of).reshape([-1 if axis == dim else 1 for axis in range(len(extent))])
    return loudness


def bell_draw(rng, extent, spread, most, shards=(), dtype=jnp.bfloat16):
    factor_of = steps_of(rng, extent, shards, -0.22, 0.18) if shards else 1.0
    array = jax.random.normal(rng, extent, jnp.float32) * spread * factor_of
    return jnp.minimum(jnp.maximum(array, -most), most).astype(dtype)


def setup_inputs(seed: int = 0) -> dict:
    key_of = jax.random.split(jax.random.key(seed), 14)
    return {
        "tokens": bell_draw(key_of[0], (TOKEN_SPAN, D), 1.0, 6.0, ((0, 8),)),
        "in_gain": jnp.clip(1.0 + 0.18 * jax.random.normal(key_of[1], (D,), jnp.float32), 0.1, 1.9),
        "query_weight": bell_draw(key_of[2], (D, KW), D ** -0.5, 0.125, ((1, 4),)),
        "key_weight": bell_draw(key_of[3], (D, KW), D ** -0.5, 0.125, ((1, 4),)),
        "value_weight": bell_draw(key_of[4], (D, VW), D ** -0.5, 0.125, ((1, 4),)),
        "gate_weight": bell_draw(key_of[5], (D, VW), D ** -0.5, 0.125, ((1, 4),)),
        "decay_down": bell_draw(key_of[6], (D, RANK), D ** -0.5, 0.125),
        "decay_up": bell_draw(key_of[7], (RANK, KW), RANK ** -0.5, 1.0),
        "decay_offset": draw_decay_offset(jax.random.fold_in(key_of[13], 71), 0),
        "decay_extra": draw_decay_extra(jax.random.fold_in(key_of[13], 71), 0),
        "head_gain": jnp.clip(1.0 + 0.18 * jax.random.normal(key_of[10], (VW,), jnp.float32), 0.1, 1.9),
        "out_weight": draw_out_weight(jax.random.fold_in(key_of[13], 71), 0),
        "out_gain": jnp.clip(1.0 + 0.18 * jax.random.normal(key_of[12], (D,), jnp.float32), 0.1, 1.9),
    }


norm_eps = 1e-06
decay_temper = 16.0

def reference(tokens, in_gain, query_weight, key_weight, value_weight, gate_weight, decay_down, decay_up, decay_offset, decay_extra, head_gain, out_weight, out_gain):
    highest = lax.Precision.HIGHEST
    tokens_wide = tokens.astype(jnp.float32)
    normed = (tokens_wide * lax.rsqrt(lax.optimization_barrier(jnp.mean(tokens_wide * tokens_wide, axis=1, keepdims=True)) + norm_eps) * in_gain).astype(jnp.bfloat16)

    def project(weight):
        return jnp.dot(normed, weight, preferred_element_type=jnp.float32).astype(jnp.bfloat16)
    query_rows = project(query_weight)
    key_rows = project(key_weight)
    value_rows = project(value_weight)
    gate_rows = project(gate_weight)
    low_rank = project(decay_down)
    logits = jnp.dot(low_rank, decay_up, preferred_element_type=jnp.float32)
    log_decay = jax.nn.log_sigmoid(logits + decay_offset) / decay_temper + decay_extra
    block_count = TOKEN_SPAN // BLOCK

    def to_blocks(values, width):
        return values.astype(jnp.float32).reshape(block_count, BLOCK, ATTENTION_UNITS, width)
    causal_mask = jnp.arange(BLOCK)[:, None] >= jnp.arange(BLOCK)[None, :]

    def block_step(carry_state, inputs):
        query_block, key_block, value_block, decay_block = inputs
        cumulative = jnp.cumsum(decay_block, axis=0)
        closing = cumulative[-1]
        query_inner = query_block * jnp.exp(cumulative)
        key_inner = key_block * jnp.exp(-cumulative)
        scores = jnp.einsum('chd,shd->hcs', query_inner, key_inner, precision=highest)
        scores = jnp.where(causal_mask[None], scores, 0.0)
        output = jnp.einsum('hcs,she->che', scores, value_block, precision=highest)
        output = output + jnp.einsum('chd,hde->che', query_inner, carry_state, precision=highest)
        key_closing = key_block * jnp.exp(closing[None] - cumulative)
        carry_state = carry_state * jnp.exp(closing)[:, :, None] + jnp.einsum('chd,che->hde', key_closing, value_block, precision=highest)
        return (carry_state, output)
    start_state = jnp.zeros((ATTENTION_UNITS, QUERY_FEATURES, DV), jnp.float32)
    final_state, outputs = lax.scan(block_step, start_state, (to_blocks(query_rows, QUERY_FEATURES), to_blocks(key_rows, QUERY_FEATURES), to_blocks(value_rows, DV), to_blocks(log_decay, QUERY_FEATURES)))
    attended = outputs.reshape(TOKEN_SPAN, ATTENTION_UNITS, DV)
    scaled = attended * lax.rsqrt(lax.optimization_barrier(jnp.mean(attended * attended, axis=2, keepdims=True)) + norm_eps) * head_gain.reshape(ATTENTION_UNITS, DV)
    gated = (scaled.reshape(TOKEN_SPAN, ATTENTION_UNITS * DV) * jax.nn.silu(gate_rows.astype(jnp.float32))).astype(jnp.bfloat16)
    mixed = jnp.dot(gated, out_weight, preferred_element_type=jnp.float32)
    result = mixed * lax.rsqrt(lax.optimization_barrier(jnp.mean(mixed * mixed, axis=1, keepdims=True)) + norm_eps) * out_gain
    return result.astype(jnp.bfloat16)
```

```python
import functools

import jax
import jax.numpy as jnp
from jax import lax
from jax.experimental import pallas as pl
from jax.experimental.pallas import tpu as pltpu
from jax.sharding import PartitionSpec as P

QUERY_FEATURES = 128
DV = 256
BLOCK = 128
PAD = 16

norm_eps = 1e-06
decay_temper = 16.0
highest = lax.Precision.HIGHEST
f32 = jnp.float32
bf16 = jnp.bfloat16
VMEM = pltpu.VMEM
ANY = pl.ANY


def mm(a, b):
    return jnp.dot(a, b, preferred_element_type=f32)


def mm_t(a, b):
    return lax.dot_general(a, b, (((1,), (1,)), ((), ())), preferred_element_type=f32)


def mm_l(a, b):
    return lax.dot_general(a, b, (((0,), (0,)), ((), ())), preferred_element_type=f32)


def kernel_a(
    heads,
    tok_hbm,
    gain_ref,
    wk_hbm,
    wv_hbm,
    down_ref,
    up_hbm,
    off_ref,
    extra_hbm,
    normed_hbm,
    k_hbm,
    v_hbm,
    c_hbm,
    *rest,
):
    msgs = rest[:heads]
    tok, wk, wv, up, extra, normed, kb, vb, cb, sems = rest[heads:]
    rows = tok.shape[0]
    width = heads * QUERY_FEATURES
    place = lax.axis_index("tp")
    columns = pl.ds(pl.multiple_of(place * width, QUERY_FEATURES), width)
    loads = [
        pltpu.make_async_copy(tok_hbm, tok, sems.at[0]),
        pltpu.make_async_copy(up_hbm.at[:, columns], up, sems.at[1]),
        pltpu.make_async_copy(extra_hbm, extra, sems.at[2]),
        pltpu.make_async_copy(wk_hbm, wk, sems.at[3]),
        pltpu.make_async_copy(wv_hbm, wv, sems.at[4]),
    ]
    for load in loads:
        load.start()
    loads[0].wait()
    gain = gain_ref[...]
    for r in range(0, rows, BLOCK):
        wide = tok[r : r + BLOCK, :].astype(f32)
        scale = lax.rsqrt(jnp.mean(wide * wide, axis=1, keepdims=True) + norm_eps)
        normed[r : r + BLOCK, :] = (wide * scale * gain).astype(bf16)
    stores = [pltpu.make_async_copy(normed, normed_hbm, sems.at[5])]
    stores[0].start()
    low = mm(normed[...], down_ref[...]).astype(bf16)
    loads[1].wait()
    loads[2].wait()
    logits = mm(low, up[...]) + off_ref[...]
    soft = jnp.minimum(logits, 0.0) - jnp.log1p(jnp.exp(-jnp.abs(logits)))
    decay = soft / decay_temper + extra[...]
    i0 = lax.broadcasted_iota(jnp.int32, (BLOCK, BLOCK), 0)
    i1 = lax.broadcasted_iota(jnp.int32, (BLOCK, BLOCK), 1)
    lower = jnp.where(i0 >= i1, 1.0, 0.0).astype(f32)
    total = jnp.zeros((1, width), f32)
    for r in range(0, rows, BLOCK):
        block = (
            lax.dot_general(
                lower,
                decay[r : r + BLOCK, :],
                (((1,), (0,)), ((), ())),
                precision=highest,
                preferred_element_type=f32,
            )
            + total
        )
        cb[r : r + BLOCK, :] = block
        total = block[BLOCK - 1 : BLOCK, :]
    stores.append(pltpu.make_async_copy(cb, c_hbm, sems.at[6]))
    stores[1].start()
    fade = jnp.exp(total - cb[...])
    closing = jnp.exp(total)
    high = closing.astype(bf16)
    rest_of = (closing - high.astype(f32)).astype(bf16)
    loads[3].wait()
    kb[...] = mm(normed[...], wk[...]).astype(bf16)
    stores.append(pltpu.make_async_copy(kb, k_hbm, sems.at[7]))
    stores[2].start()
    faded = (kb[...].astype(f32) * fade).astype(bf16)
    loads[4].wait()
    row = lax.broadcasted_iota(jnp.int32, (PAD, QUERY_FEATURES), 0)
    for h in range(heads):
        cv = slice(h * DV, (h + 1) * DV)
        ck = slice(h * QUERY_FEATURES, (h + 1) * QUERY_FEATURES)
        vb[:, cv] = mm(normed[...], wv[:, cv]).astype(bf16)
        msgs[h][:DV, :] = mm_l(vb[:, cv], faded[:, ck]).astype(bf16)
        tail = jnp.where(
            row == 0,
            high[:, ck].astype(f32),
            jnp.where(row == 1, rest_of[:, ck].astype(f32), 0.0),
        )
        msgs[h][DV:, :] = tail.astype(bf16)
    stores.append(pltpu.make_async_copy(vb, v_hbm, sems.at[8]))
    stores[3].start()
    for store in stores:
        store.wait()


def local_states(
    tokens, in_gain, key_weight, value_weight, decay_down, decay_up, decay_offset, decay_extra
):
    rows, model = tokens.shape
    width = key_weight.shape[1]
    values = value_weight.shape[1]
    heads = width // QUERY_FEATURES
    out_shape = [
        jax.ShapeDtypeStruct((rows, model), bf16),
        jax.ShapeDtypeStruct((rows, width), bf16),
        jax.ShapeDtypeStruct((rows, values), bf16),
        jax.ShapeDtypeStruct((rows, width), f32),
    ] + [jax.ShapeDtypeStruct((DV + PAD, QUERY_FEATURES), bf16)] * heads
    vm = pl.BlockSpec(memory_space=VMEM)
    hb = pl.BlockSpec(memory_space=ANY)
    return pl.pallas_call(
        functools.partial(kernel_a, heads),
        out_shape=out_shape,
        in_specs=[hb, vm, hb, hb, vm, hb, vm, hb],
        out_specs=[hb] * 4 + [vm] * heads,
        scratch_shapes=[
            VMEM((rows, model), bf16),
            VMEM((model, width), bf16),
            VMEM((model, values), bf16),
            VMEM((decay_up.shape[0], width), bf16),
            VMEM((rows, width), f32),
            VMEM((rows, model), bf16),
            VMEM((rows, width), bf16),
            VMEM((rows, values), bf16),
            VMEM((rows, width), f32),
            pltpu.SemaphoreType.DMA((9,)),
        ],
        compiler_params=pltpu.CompilerParams(vmem_limit_bytes=24 << 20),
        cost_estimate=pl.CostEstimate(
            flops=2 * rows * model * (width + values), bytes_accessed=8 << 20, transcendentals=0
        ),
        name="states",
    )(
        tokens,
        in_gain[None, :],
        key_weight,
        value_weight,
        decay_down,
        decay_up,
        decay_offset[None, :],
        decay_extra,
    )


def kernel_b(heads, normed, wq, wg, k, v, c, gain, *outs):
    locals_, queries, gates = outs[:heads], outs[heads : 2 * heads], outs[2 * heads :]
    rows = normed.shape[0]
    i0 = lax.broadcasted_iota(jnp.int32, (BLOCK, BLOCK), 0)
    i1 = lax.broadcasted_iota(jnp.int32, (BLOCK, BLOCK), 1)
    causal = i0 >= i1
    q_all = mm(normed[...], wq[...]).astype(bf16).astype(f32)
    for h in range(heads):
        ck = slice(h * QUERY_FEATURES, (h + 1) * QUERY_FEATURES)
        cv = slice(h * DV, (h + 1) * DV)
        q_head = q_all[:, ck]
        state = None
        start = None
        for r in range(0, rows, BLOCK):
            rs = slice(r, r + BLOCK)
            q = q_head[rs, :]
            kk = k[rs, ck].astype(f32)
            vv = v[rs, cv]
            cc = c[rs, ck]
            middle = c[r + BLOCK // 2 - 1 : r + BLOCK // 2, ck]
            end = c[r + BLOCK - 1 : r + BLOCK, ck]
            queries[h][rs, :] = (q * jnp.exp(cc)).astype(bf16)
            q_mid = (q * jnp.exp(cc - middle)).astype(bf16)
            k_mid = (kk * jnp.exp(middle - cc)).astype(bf16)
            scores = jnp.where(causal, mm_t(q_mid, k_mid), 0.0).astype(bf16)
            out = mm(scores, vv)
            if state is not None:
                out = out + mm_t((q * jnp.exp(cc - start)).astype(bf16), state.astype(bf16))
            locals_[h][rs, :] = out
            if r + BLOCK < rows:
                k_end = (kk * jnp.exp(end - cc)).astype(bf16)
                added = mm_l(vv, k_end)
                state = added if state is None else state * jnp.exp(end - start) + added
                start = end
        gate = mm(normed[...], wg[:, cv]).astype(bf16).astype(f32)
        gates[h][...] = gain[:, cv] * (gate * jax.nn.sigmoid(gate))


def local_attention(normed, query_weight, gate_weight, k, v, c, head_gain):
    rows, model = normed.shape
    width = query_weight.shape[1]
    values = gate_weight.shape[1]
    heads = width // QUERY_FEATURES
    vm = pl.BlockSpec(memory_space=VMEM)
    return pl.pallas_call(
        functools.partial(kernel_b, heads),
        out_shape=[jax.ShapeDtypeStruct((rows, DV), f32)] * heads
        + [jax.ShapeDtypeStruct((rows, QUERY_FEATURES), bf16)] * heads
        + [jax.ShapeDtypeStruct((rows, DV), f32)] * heads,
        in_specs=[vm] * 7,
        out_specs=[vm] * (3 * heads),
        compiler_params=pltpu.CompilerParams(vmem_limit_bytes=24 << 20),
        cost_estimate=pl.CostEstimate(
            flops=2 * rows * model * (width + values), bytes_accessed=8 << 20, transcendentals=0
        ),
        name="attention",
    )(normed, query_weight, gate_weight, k, v, c, head_gain[None, :])


def kernel_c(loc, q, state, gate, out):
    att = loc[...] + mm_t(q[...], state[...])
    scale = lax.rsqrt(jnp.mean(att * att, axis=1, keepdims=True) + norm_eps)
    out[...] = (att * scale * gate[...]).astype(bf16)


def finish_head(loc, q, state, gate):
    vm = pl.BlockSpec(memory_space=VMEM)
    return pl.pallas_call(
        kernel_c,
        out_shape=jax.ShapeDtypeStruct(loc.shape, bf16),
        in_specs=[vm] * 4,
        out_specs=vm,
        compiler_params=pltpu.CompilerParams(vmem_limit_bytes=8 << 20),
        cost_estimate=pl.CostEstimate(
            flops=2 * loc.shape[0] * DV * QUERY_FEATURES, bytes_accessed=1 << 20, transcendentals=0
        ),
        name="finish",
    )(loc, q, state, gate)


def swap(value, axis, count, bit):
    return lax.ppermute(value, axis, [(i, i ^ bit) for i in range(count)])


def turn(value, axis, count, by):
    return lax.ppermute(value, axis, [(i, (i + by) % count) for i in range(count)])


def split(message):
    decay = message[DV : DV + 1].astype(f32) + message[DV + 1 : DV + 2].astype(f32)
    return message[:DV].astype(f32), decay


def join(state, decay):
    high = decay.astype(bf16)
    low = (decay - high.astype(f32)).astype(bf16)
    pad = jnp.zeros((PAD - 2, decay.shape[1]), bf16)
    return jnp.concatenate([state.astype(bf16), high, low, pad], axis=0)


def entering(messages, count):
    place = lax.axis_index("sp")
    totals = list(messages)
    heads = len(totals)
    entered = [None] * heads
    before = [None] * heads
    bit = 1
    while bit < count:
        later = (place & bit) != 0
        received = [swap(m, "sp", count, bit) for m in totals]
        for h in range(heads):
            state, decay = split(received[h])
            own_state, own_decay = split(totals[h])
            if entered[h] is None:
                entered[h] = jnp.where(later, state, 0.0)
                before[h] = jnp.where(later, decay, 1.0)
            else:
                entered[h] = jnp.where(later, entered[h] + before[h] * state, entered[h])
                before[h] = jnp.where(later, before[h] * decay, before[h])
            if 2 * bit < count:
                totals[h] = join(
                    jnp.where(later, own_decay * state + own_state, decay * own_state + state),
                    own_decay * decay,
                )
        bit *= 2
    return [e.astype(bf16) for e in entered]


def local(
    sp,
    tp,
    tokens,
    in_gain,
    query_weight,
    key_weight,
    value_weight,
    gate_weight,
    decay_down,
    decay_up,
    decay_offset,
    decay_extra,
    head_gain,
    out_weight,
    out_gain,
):
    heads = query_weight.shape[1] // QUERY_FEATURES
    values = value_weight.shape[1]
    normed, k, v, c, *messages = local_states(
        tokens, in_gain, key_weight, value_weight, decay_down, decay_up, decay_offset, decay_extra
    )
    outs = local_attention(normed, query_weight, gate_weight, k, v, c, head_gain)
    locals_, queries, gates = outs[:heads], outs[heads : 2 * heads], outs[2 * heads :]
    states = entering(messages, sp)
    place = lax.axis_index("tp")
    mixed = 0.0
    for h in range(heads):
        gated = finish_head(locals_[h], queries[h], states[h], gates[h])

        def add(mixed, piece, owner):
            start = owner * values + h * DV
            rows_of = lax.dynamic_slice_in_dim(out_weight, start, DV, 0)
            return mixed + mm(piece, rows_of)

        mixed = add(mixed, gated, place)
        mixed = add(mixed, swap(gated, "tp", tp, 1), place ^ 1)
        for by in range(2, tp, 2):
            piece = turn(gated, "tp", tp, by)
            owner = (place - by) % tp
            mixed = add(mixed, piece, owner)
            mixed = add(mixed, swap(piece, "tp", tp, 1), owner ^ 1)
    squares = jnp.sum(mixed * mixed, axis=1, keepdims=True)
    part = squares.reshape(-1, QUERY_FEATURES)
    whole = part
    for by in range(1, tp):
        whole = whole + turn(part, "tp", tp, by)
    squares = whole.reshape(-1, 1)
    out_width = tp * out_weight.shape[1]
    result = mixed * lax.rsqrt(squares / out_width + norm_eps) * out_gain
    return result.astype(bf16)


def solution(mesh):
    placed = (
        P("sp", None),
        P(),
        P(None, "tp"),
        P(None, "tp"),
        P(None, "tp"),
        P(None, "tp"),
        P(),
        P(),
        P("tp"),
        P("sp", "tp"),
        P("tp"),
        P(None, "tp"),
        P("tp"),
    )
    return jax.shard_map(
        functools.partial(local, mesh.shape["sp"], mesh.shape["tp"]),
        mesh=mesh,
        in_specs=placed,
        out_specs=P("sp", "tp"),
        check_vma=False,
    )
```
